32 devices in a mesh: fs: 4 (over z), rep: 4 (over y, x), tp: 2 (over core).
Axes of the slice: x: 2, y: 2, z: 4, core: 2. Of those that a mesh axis runs over, the one named last changes fastest.
Arguments:
- saved_input: bfloat16 [16384, 2048], P(('fs', 'rep')), may hold values from -6 to 6
- cot_input: bfloat16 [16384, 1024], P(('fs', 'rep'), 'tp'), may hold values from -0.046875 to 0.046875
- cot_gate: bfloat16 [16384, 1024], P(('fs', 'rep'), 'tp'), may hold values from -0.046875 to 0.046875
- in_master: float32 [2048, 1024], P('fs', 'tp'), may hold values from -3 to 3
- gate_master: float32 [2048, 1024], P('fs', 'tp'), may hold values from -3 to 3
- in_factor: bfloat16 [2048, 256], P('fs'), may hold values from -0.125 to 0.125
- gate_factor: bfloat16 [2048, 256], P('fs'), may hold values from -0.125 to 0.125
- in_first: float32 [256, 1024], P('fs', 'tp'), may hold values from -6 to 6
- in_second: float32 [256, 1024], P('fs', 'tp'), may hold values from 0.5 to 2
- gate_first: float32 [256, 1024], P('fs', 'tp'), may hold values from -6 to 6
- gate_second: float32 [256, 1024], P('fs', 'tp'), may hold values from 0.5 to 2
Outputs:
- in_master_new: float32 [2048, 1024], P('fs', 'tp')
- gate_master_new: float32 [2048, 1024], P('fs', 'tp')
- in_update: float32 [2048, 1024], P('fs', 'tp')
- gate_update: float32 [2048, 1024], P('fs', 'tp')
- in_first_new: float32 [256, 1024], P('fs', 'tp')
- in_second_new: float32 [256, 1024], P('fs', 'tp')
- gate_first_new: float32 [256, 1024], P('fs', 'tp')
- gate_second_new: float32 [256, 1024], P('fs', 'tp')
- in_copy: bfloat16 [2048, 1024], P(None, 'tp')
- gate_copy: bfloat16 [2048, 1024], P(None, 'tp')
The draws below stay inside these ranges and needn't reach their ends.
All inputs are finite; a program needn't handle non-finite values.
Results may differ from the reference program's by a relative error of at most 0.0065.
Values may be sent and summed in bfloat16 or wider, within the bound.
A program may use at most 64 MiB of HBM per device.

```python
import math
import jax
import jax.numpy as jnp
from jax import lax

D = 2048
W = 1024
RANK = 256
TOKENS = 16384


def steps_of(own_key, shape, pieces, low, top_value):
    level, own = 1.0, jax.random.fold_in(own_key, 6)
    for position, parts in pieces:
        steps = jnp.exp(jax.random.uniform(jax.random.fold_in(own, position), (parts,), jnp.float32, low / len(pieces), top_value / len(pieces)))
        level = level * jnp.repeat(steps, shape[position] // parts).reshape([-1 if axis == position else 1 for axis in range(len(shape))])
    return level


def gaussian(rng, shape, scale, reach, shards=(), kind=jnp.bfloat16):
    gain = steps_of(rng, shape, shards, -0.22, 0.18) if shards else 1.0
    entries = jax.random.normal(rng, shape, jnp.float32) * scale * gain
    return jnp.minimum(jnp.maximum(entries, -reach), reach).astype(kind)


def setup_inputs(seed: int = 0) -> dict:
    keys = jax.random.split(jax.random.key(seed), 12)
    saved_input = gaussian(keys[0], (TOKENS, D), 1.0, 6.0, ((0, 16),))
    cot_input = gaussian(keys[1], (TOKENS, W), TOKENS ** -0.5, 0.046875, ((0, 16), (1, 2)))
    cot_gate = gaussian(keys[2], (TOKENS, W), TOKENS ** -0.5, 0.046875, ((0, 16), (1, 2)))
    in_master = gaussian(keys[3], (D, W), 0.5, 3.0, ((0, 4), (1, 2)), jnp.float32)
    gate_master = gaussian(keys[4], (D, W), 0.5, 3.0, ((0, 4), (1, 2)), jnp.float32)
    in_factor = gaussian(keys[5], (D, RANK), D ** -0.5, 0.125, ((0, 4),))
    gate_factor = gaussian(keys[6], (D, RANK), D ** -0.5, 0.125, ((0, 4),))
    in_first = gaussian(keys[7], (RANK, W), 1.0, 6.0, ((0, 4), (1, 2)), jnp.float32)
    in_second = jnp.clip(jnp.exp(math.log(2.0) - 1.3862944 * jax.random.uniform(keys[8], (RANK, W), jnp.float32) ** steps_of(keys[8], (RANK, W), ((0, 4), (1, 2)), -0.2, 0.2)), 0.5, 2.0)
    gate_first = gaussian(keys[9], (RANK, W), 1.0, 6.0, ((0, 4), (1, 2)), jnp.float32)
    gate_second = jnp.clip(jnp.exp(math.log(2.0) - 1.3862944 * jax.random.uniform(keys[10], (RANK, W), jnp.float32) ** steps_of(keys[10], (RANK, W), ((0, 4), (1, 2)), -0.2, 0.2)), 0.5, 2.0)
    return {"saved_input": saved_input, "cot_input": cot_input, "cot_gate": cot_gate, "in_master": in_master, "gate_master": gate_master, "in_factor": in_factor, "gate_factor": gate_factor, "in_first": in_first, "in_second": in_second, "gate_first": gate_first, "gate_second": gate_second}


def adapt(grad, master, factor, first, second):
    basis = factor.astype(jnp.float32)
    low = jnp.dot(basis.T, grad, precision=lax.Precision.HIGHEST)
    first_new = 0.8 * first + 0.2 * low
    second_new = 0.95 * second + 0.05 * low * low
    normed = first_new / jnp.sqrt(second_new)
    full = jnp.dot(basis, normed, precision=lax.Precision.HIGHEST)
    square = jnp.sum(full * full)
    update = full / jnp.sqrt(square / (D * W) + 0.1)
    master_new = master - 0.05 * update
    return (master_new, update, first_new, second_new, master_new.astype(jnp.bfloat16))

def reference(saved_input, cot_input, cot_gate, in_master, gate_master, in_factor, gate_factor, in_first, in_second, gate_first, gate_second):
    cotangents = jnp.concatenate([cot_input, cot_gate], axis=1)
    span = math.gcd(TOKENS, 8192)
    inputs = saved_input.reshape(TOKENS // span, span, D)
    grads_in = cotangents.reshape(TOKENS // span, span, 2 * W)

    def accumulate(total, pair):
        rows, cots = pair
        part = jnp.dot(rows.astype(jnp.float32).T, cots.astype(jnp.float32), precision=lax.Precision.HIGHEST)
        return (total + part, None)
    grads, _ = lax.scan(accumulate, jnp.zeros((D, 2 * W), jnp.float32), (inputs, grads_in))
    in_out = adapt(grads[:, :W], in_master, in_factor, in_first, in_second)
    gate_out = adapt(grads[:, W:], gate_master, gate_factor, gate_first, gate_second)
    return (in_out[0], gate_out[0], in_out[1], gate_out[1], in_out[2], in_out[3], gate_out[2], gate_out[3], in_out[4], gate_out[4])
```

```python
import functools

import jax
import jax.numpy as jnp
from jax import lax
from jax.experimental import pallas as pl
from jax.experimental.pallas import tpu as pltpu
from jax.sharding import PartitionSpec as P

MESH = pl.DeviceIdType.MESH
BF = jnp.bfloat16
F32 = jnp.float32
LIMIT = 60 * 1024 * 1024


def exchange_kernel(
    n_f, n_r,
    x_hbm, ci_hbm, cg_hbm, mi_hbm, mg_hbm, fi_hbm, fg_hbm, p0_hbm, s0_hbm, p1_hbm, s1_hbm,
    masters_out, factor_out, normed_out, low_out, square_out,
    x_v, cot_v, fac, mas32, mas16, old, acc, pbuf, r1buf, sumbuf, r2buf, nall, lall, sq,
    loc, f1s, f1r, f2s, f2r, f3s, f3r, m1s, m1r, m2s, m2r, r1s, r1r, r2s, r2r,
    a1s, a1r, als, alr, a2s, a2r, sqs, sqr,
):
    f, r, t = lax.axis_index("fs"), lax.axis_index("rep"), lax.axis_index("tp")
    tokens = x_v.shape[0]
    rows = mi_hbm.shape[0]
    width = mi_hbm.shape[1]
    rank = fi_hbm.shape[1]
    own = p0_hbm.shape[0]
    cw = width // n_r
    half = rows // 2
    piece = half // n_r
    quarter = rows // n_r
    ks = sorted(range(1, n_f), key=lambda k: min(k, n_f - k))
    js = list(range(1, n_r))

    def f_to(k):
        return lax.rem(f + k, n_f)

    def f_from(k):
        return lax.rem(f - k + n_f, n_f)

    def r_to(j):
        return lax.rem(r + j, n_r)

    def span(start, size, unit):
        return pl.ds(pl.multiple_of(start, unit), size)

    sent = []

    def send(src, dst, ss, rs, ff, rr, tt):
        c = pltpu.make_async_remote_copy(
            src_ref=src, dst_ref=dst, send_sem=ss, recv_sem=rs,
            device_id=(ff, rr, tt), device_id_type=MESH)
        c.start()
        sent.append(c)
        return c

    def local(src, dst, i):
        c = pltpu.make_async_copy(src, dst, loc.at[i])
        c.start()
        return c

    mine = span(f * rows, rows, rows)
    lf = [local(fi_hbm, fac.at[mine, pl.ds(0, rank)], 0), local(fg_hbm, fac.at[mine, pl.ds(rank, rank)], 1)]
    lm = [local(mi_hbm, mas32.at[0], 2), local(mg_hbm, mas32.at[1], 3)]
    lx = local(x_hbm, x_v, 4)
    lc = [local(ci_hbm, cot_v.at[0], 5), local(cg_hbm, cot_v.at[1], 6)]
    lo = [local(h, old.at[i], 7 + i) for i, h in enumerate((p0_hbm, s0_hbm, p1_hbm, s1_hbm))]

    barrier = pltpu.get_barrier_semaphore()
    for k in ks:
        pl.semaphore_signal(barrier, inc=1, device_id=(f_to(k), r, t), device_id_type=MESH)
    for j in js:
        pl.semaphore_signal(barrier, inc=1, device_id=(f, r_to(j), t), device_id_type=MESH)
    pl.semaphore_signal(barrier, inc=1, device_id=(f, r, 1 - t), device_id_type=MESH)
    pl.semaphore_wait(barrier, len(ks) + len(js) + 1)

    for c in lf:
        c.wait()
    f1 = {}
    for k in ks:
        at = span(f * rows + t * half + r * piece, piece, piece)
        f1[k] = send(fac.at[at], fac.at[at], f1s.at[k], f1r.at[k], f_to(k), r, t)
    for c in lm:
        c.wait()
    for g in range(2):
        mas16[:, g * width:(g + 1) * width] = mas32[g].astype(BF)
    m1 = {}
    for k in ks:
        m1[k] = send(
            mas16.at[span(r * quarter, quarter, quarter)],
            masters_out.at[span(f * rows + r * quarter, quarter, quarter)],
            m1s.at[k], m1r.at[k], f_to(k), r, t)
    lown = local(mas16, masters_out.at[mine], 11)
    lx.wait()

    tile = min(256, tokens)

    blocked = rows % 128 == 0

    def project(source, first):
        if not blocked and not first:
            return
        depth = span(source * rows, rows, rows) if blocked else slice(None)
        weights = fac[depth, :]

        def step(i, carry):
            at = span(i * tile, tile, tile)
            part = jnp.dot(x_v[at, depth], weights, preferred_element_type=F32)
            acc[at, :] = part if first else acc[at, :] + part
            return carry

        lax.fori_loop(0, tokens // tile, step, 0)

    f2 = {}

    def spread(k):
        f1[k].wait_recv()
        at = span(f_from(k) * rows + t * half + r * piece, piece, piece)
        for j in js:
            f2[k, j] = send(fac.at[at], fac.at[at], f2s.at[k, j], f2r.at[k, j], f, r_to(j), t)

    if blocked:
        project(f, True)
    for k in ks:
        spread(k)
    f3 = {}
    for k in ks:
        for j in js:
            f2[k, j].wait_recv()
        at = span(f_from(k) * rows + t * half, half, half)
        f3[k] = send(fac.at[at], fac.at[at], f3s.at[k], f3r.at[k], f, r, 1 - t)
    for k in ks:
        f3[k].wait_recv()
        project(f_from(k), False)
    if not blocked:
        project(f, True)
    lfac = local(fac, factor_out, 12)

    for c in lc:
        c.wait()
    r1 = {}
    for g in range(2):
        turned = acc[:, g * rank:(g + 1) * rank].astype(BF).T
        part = jnp.dot(turned, cot_v[g], preferred_element_type=F32).astype(BF)
        for q in range(n_r):
            pbuf[q, g] = part[:, q * cw:(q + 1) * cw]
        for j in js:
            r1[j, g] = send(pbuf.at[r_to(j), g], r1buf.at[j, g], r1s.at[j, g], r1r.at[j, g], f, r_to(j), t)

    m2 = {}

    def spread_masters(k):
        m1[k].wait_recv()
        at = span(f_from(k) * rows + r * quarter, quarter, quarter)
        for j in js:
            m2[k, j] = send(masters_out.at[at], masters_out.at[at], m2s.at[k, j], m2r.at[k, j], f, r_to(j), t)

    cut1 = (len(ks) + 2) // 3
    cut2 = (2 * len(ks) + 2) // 3
    for k in ks[:cut1]:
        spread_masters(k)

    for g in range(2):
        total = pbuf[r, g].astype(F32)
        for j in js:
            r1[j, g].wait_recv()
            total = total + r1buf[j, g].astype(F32)
        sumbuf[g] = total.astype(BF)
    r2 = {}
    for k in ks:
        r2[k] = send(
            sumbuf.at[:, span(f_to(k) * own, own, own), :], r2buf.at[k],
            r2s.at[k], r2r.at[k], f_to(k), r, t)
    low = sumbuf[:, span(f * own, own, own), :].astype(F32)
    for k in ks:
        r2[k].wait_recv()
        low = low + r2buf[k].astype(F32)
    for c in lo:
        c.wait()
    lall[r] = low.astype(BF)
    columns = span(r * cw, cw, cw)
    for g in range(2):
        first = 0.8 * old[2 * g, :, columns] + 0.2 * low[g]
        second = 0.95 * old[2 * g + 1, :, columns] + 0.05 * low[g] * low[g]
        nall[r, g, span(f * own, own, own), :] = (first / jnp.sqrt(second)).astype(BF)
    a1 = {}
    for k in ks:
        at = nall.at[r, :, span(f * own, own, own), :]
        a1[k] = send(at, at, a1s.at[k], a1r.at[k], f_to(k), r, t)
    al = {}
    for j in js:
        al[j] = send(lall.at[r], lall.at[r], als.at[j], alr.at[j], f, r_to(j), t)
    for k in ks[cut1:cut2]:
        spread_masters(k)
    for k in ks:
        a1[k].wait_recv()
    a2 = {}
    for j in js:
        a2[j] = send(nall.at[r], nall.at[r], a2s.at[j], a2r.at[j], f, r_to(j), t)
    for k in ks[cut2:]:
        spread_masters(k)
    for j in js:
        al[j].wait_recv()
    llow = local(lall, low_out, 13)
    for j in js:
        a2[j].wait_recv()
    lnorm = local(nall, normed_out, 14)

    for g in range(2):
        whole = jnp.concatenate([nall[q, g] for q in range(n_r)], axis=1)

        def square(i, total):
            at = span(i * 256, 256, 256)
            full = jnp.dot(fac[at, g * rank:(g + 1) * rank], whole, preferred_element_type=F32)
            return total + jnp.sum((full * full).reshape(32, 8, width), axis=0)

        total = lax.fori_loop(0, fac.shape[0] // 256, square, jnp.zeros((8, width), F32))
        part = total[:, :128]
        for q in range(1, width // 128):
            part = part + total[:, q * 128:(q + 1) * 128]
        sq[t, g] = part
    other = send(sq.at[t], sq.at[t], sqs, sqr, f, r, 1 - t)
    other.wait_recv()
    lsq = local(sq, square_out, 15)
    for c in (lown, lfac, llow, lnorm, lsq):
        c.wait()
    for k in ks:
        for j in js:
            m2[k, j].wait_recv()
    for c in sent:
        c.wait_send()


def finish_kernel(
    entries,
    fac, mas, nor, low, sqr, fi, fg, mi, mg, p0, s0, p1, s1,
    mi_new, mg_new, ui, ug, p0n, s0n, p1n, s1n, ci, cg,
):
    n_r = nor.shape[0]
    width = mi.shape[1]
    rank = fi.shape[1]
    new = ((p0, s0, p0n, s0n), (p1, s1, p1n, s1n))

    @pl.when(pl.program_id(0) == 0)
    def _():
        for g, (p, s, pn, sn) in enumerate(new):
            got = jnp.concatenate([low[q, g] for q in range(n_r)], axis=1).astype(F32)
            pn[...] = 0.8 * p[...] + 0.2 * got
            sn[...] = 0.95 * s[...] + 0.05 * got * got

    for g, (own_f, own_m, m_new, up, copy) in enumerate(((fi, mi, mi_new, ui, ci), (fg, mg, mg_new, ug, cg))):
        whole = jnp.concatenate([nor[q, g] for q in range(n_r)], axis=1)
        square = jnp.sum(sqr[0, g] + sqr[1, g], keepdims=True)
        scale = 1.0 / jnp.sqrt(square / entries + 0.1)
        full = jnp.dot(own_f[...], whole, preferred_element_type=F32)
        update = full * scale
        up[...] = update
        m_new[...] = own_m[...] - 0.05 * update
        rest = jnp.dot(fac[:, g * rank:(g + 1) * rank], whole, preferred_element_type=F32)
        base = mas[:, g * width:(g + 1) * width].astype(F32)
        copy[...] = (base - 0.05 * (rest * scale)).astype(BF)


def on_device(n_f, n_r, n_t, x, ci, cg, mi, mg, fi, fg, p0, s0, p1, s1):
    tokens, d = x.shape
    rows, width = mi.shape
    rank = fi.shape[1]
    own = p0.shape[0]
    cw = width // n_r
    any_ = pl.BlockSpec(memory_space=pl.ANY)
    dma = pltpu.SemaphoreType.DMA
    S = jax.ShapeDtypeStruct
    masters, factors, normed, low, squares = pl.pallas_call(
        functools.partial(exchange_kernel, n_f, n_r),
        out_shape=(
            S((d, 2 * width), BF),
            S((d, 2 * rank), BF),
            S((n_r, 2, rank, cw), BF),
            S((n_r, 2, own, cw), BF),
            S((2, 2, 8, 128), F32),
        ),
        in_specs=[any_] * 11,
        out_specs=(any_,) * 5,
        scratch_shapes=[
            pltpu.VMEM((tokens, d), BF),
            pltpu.VMEM((2, tokens, width), BF),
            pltpu.VMEM((d, 2 * rank), BF),
            pltpu.VMEM((2, rows, width), F32),
            pltpu.VMEM((rows, 2 * width), BF),
            pltpu.VMEM((4, own, width), F32),
            pltpu.VMEM((tokens, 2 * rank), F32),
            pltpu.VMEM((n_r, 2, rank, cw), BF),
            pltpu.VMEM((n_r, 2, rank, cw), BF),
            pltpu.VMEM((2, rank, cw), BF),
            pltpu.VMEM((n_f, 2, own, cw), BF),
            pltpu.VMEM((n_r, 2, rank, cw), BF),
            pltpu.VMEM((n_r, 2, own, cw), BF),
            pltpu.VMEM((2, 2, 8, 128), F32),
            dma((16,)),
            dma((n_f,)), dma((n_f,)),
            dma((n_f, n_r)), dma((n_f, n_r)),
            dma((n_f,)), dma((n_f,)),
            dma((n_f,)), dma((n_f,)),
            dma((n_f, n_r)), dma((n_f, n_r)),
            dma((n_r, 2)), dma((n_r, 2)),
            dma((n_f,)), dma((n_f,)),
            dma((n_f,)), dma((n_f,)),
            dma((n_r,)), dma((n_r,)),
            dma((n_r,)), dma((n_r,)),
            dma, dma,
        ],
        compiler_params=pltpu.CompilerParams(
            collective_id=0, has_side_effects=True, vmem_limit_bytes=LIMIT),
        name="exchange",
    )(x, ci, cg, mi, mg, fi, fg, p0, s0, p1, s1)

    steps = 8
    dt, rt = d // steps, rows // steps

    def tiled(a, b):
        return pl.BlockSpec((a, b), lambda i: (i, 0))

    def fixed(shape):
        return pl.BlockSpec(shape, lambda i: (0,) * len(shape))

    moment = fixed((own, width))
    return pl.pallas_call(
        functools.partial(finish_kernel, d * width * n_t),
        grid=(steps,),
        out_shape=(S((rows, width), F32),) * 4 + (S((own, width), F32),) * 4 + (S((d, width), BF),) * 2,
        in_specs=[
            tiled(dt, 2 * rank), tiled(dt, 2 * width),
            fixed(normed.shape), fixed(low.shape), fixed(squares.shape),
            tiled(rt, rank), tiled(rt, rank), tiled(rt, width), tiled(rt, width),
            moment, moment, moment, moment,
        ],
        out_specs=(tiled(rt, width),) * 4 + (moment,) * 4 + (tiled(dt, width),) * 2,
        compiler_params=pltpu.CompilerParams(
            dimension_semantics=("arbitrary",), vmem_limit_bytes=LIMIT // 2),
        name="finish",
    )(factors, masters, normed, low, squares, fi, fg, mi, mg, p0, s0, p1, s1)


def solution(mesh):
    tokens = P(("fs", "rep"), None)
    cots = P(("fs", "rep"), "tp")
    both, tall, wide = P("fs", "tp"), P("fs", None), P(None, "tp")
    return jax.shard_map(
        functools.partial(on_device, mesh.shape["fs"], mesh.shape["rep"], mesh.shape["tp"]),
        mesh=mesh,
        in_specs=(tokens, cots, cots, both, both, tall, tall, both, both, both, both),
        out_specs=(both,) * 8 + (wide,) * 2,
        check_vma=False,
    )
```

```python
import functools

import jax
import jax.numpy as jnp
from jax import lax
from jax.experimental import pallas as pl
from jax.experimental.pallas import tpu as pltpu
from jax.sharding import PartitionSpec as P

MESH = pl.DeviceIdType.MESH
BF = jnp.bfloat16
F32 = jnp.float32
LIMIT = 60 * 1024 * 1024


def exchange_kernel(
    n_f, n_r,
    x_hbm, ci_hbm, cg_hbm, mi_hbm, mg_hbm, fi_hbm, fg_hbm, p0_hbm, s0_hbm, p1_hbm, s1_hbm,
    masters_out, factor_out, normed_out, low_out, square_out,
    x_v, cot_v, fac, mas32, mas16, old, acc, pbuf, r1buf, sumbuf, r2buf, nall, lall, sq,
    loc, f1s, f1r, f2s, f2r, f3s, f3r, m1s, m1r, m2s, m2r, r1s, r1r, r2s, r2r,
    a1s, a1r, als, alr, a2s, a2r, sqs, sqr,
):
    f, r, t = lax.axis_index("fs"), lax.axis_index("rep"), lax.axis_index("tp")
    tokens = x_v.shape[0]
    rows = mi_hbm.shape[0]
    width = mi_hbm.shape[1]
    rank = fi_hbm.shape[1]
    own = p0_hbm.shape[0]
    cw = width // n_r
    half = rows // 2
    piece = half // n_r
    quarter = rows // n_r
    ks = sorted(range(1, n_f), key=lambda k: min(k, n_f - k))
    js = list(range(1, n_r))

    def f_to(k):
        return lax.rem(f + k, n_f)

    def f_from(k):
        return lax.rem(f - k + n_f, n_f)

    def r_to(j):
        return lax.rem(r + j, n_r)

    def span(start, size, unit):
        return pl.ds(pl.multiple_of(start, unit), size)

    sent = []

    def send(src, dst, ss, rs, ff, rr, tt):
        c = pltpu.make_async_remote_copy(
            src_ref=src, dst_ref=dst, send_sem=ss, recv_sem=rs,
            device_id=(ff, rr, tt), device_id_type=MESH)
        c.start()
        sent.append(c)
        return c

    def local(src, dst, i):
        c = pltpu.make_async_copy(src, dst, loc.at[i])
        c.start()
        return c

    mine = span(f * rows, rows, rows)
    lf = [local(fi_hbm, fac.at[mine, pl.ds(0, rank)], 0), local(fg_hbm, fac.at[mine, pl.ds(rank, rank)], 1)]
    lm = [local(mi_hbm, mas32.at[0], 2), local(mg_hbm, mas32.at[1], 3)]
    lx = local(x_hbm, x_v, 4)
    lc = [local(ci_hbm, cot_v.at[0], 5), local(cg_hbm, cot_v.at[1], 6)]
    lo = [local(h, old.at[i], 7 + i) for i, h in enumerate((p0_hbm, s0_hbm, p1_hbm, s1_hbm))]

    barrier = pltpu.get_barrier_semaphore()
    for k in ks:
        pl.semaphore_signal(barrier, inc=1, device_id=(f_to(k), r, t), device_id_type=MESH)
    for j in js:
        pl.semaphore_signal(barrier, inc=1, device_id=(f, r_to(j), t), device_id_type=MESH)
    pl.semaphore_signal(barrier, inc=1, device_id=(f, r, 1 - t), device_id_type=MESH)
    pl.semaphore_wait(barrier, len(ks) + len(js) + 1)

    for c in lf:
        c.wait()
    f1 = {}
    for k in ks:
        at = span(f * rows + t * half + r * piece, piece, piece)
        f1[k] = send(fac.at[at], fac.at[at], f1s.at[k], f1r.at[k], f_to(k), r, t)
    for c in lm:
        c.wait()
    for g in range(2):
        mas16[:, g * width:(g + 1) * width] = mas32[g].astype(BF)
    m1 = {}
    for k in ks:
        m1[k] = send(
            mas16.at[span(r * quarter, quarter, quarter)],
            masters_out.at[span(f * rows + r * quarter, quarter, quarter)],
            m1s.at[k], m1r.at[k], f_to(k), r, t)
    lown = local(mas16, masters_out.at[mine], 11)
    lx.wait()

    tile = min(256, tokens)

    blocked = rows % 128 == 0

    def project(source, first):
        if not blocked and not first:
            return
        depth = span(source * rows, rows, rows) if blocked else slice(None)
        weights = fac[depth, :]

        def step(i, carry):
            at = span(i * tile, tile, tile)
            part = jnp.dot(x_v[at, depth], weights, preferred_element_type=F32)
            acc[at, :] = part if first else acc[at, :] + part
            return carry

        lax.fori_loop(0, tokens // tile, step, 0)

    f2 = {}

    def spread(k):
        f1[k].wait_recv()
        at = span(f_from(k) * rows + t * half + r * piece, piece, piece)
        for j in js:
            f2[k, j] = send(fac.at[at], fac.at[at], f2s.at[k, j], f2r.at[k, j], f, r_to(j), t)

    if blocked:
        project(f, True)
    for k in ks:
        spread(k)
    f3 = {}
    for k in ks:
        for j in js:
            f2[k, j].wait_recv()
        at = span(f_from(k) * rows + t * half, half, half)
        f3[k] = send(fac.at[at], fac.at[at], f3s.at[k], f3r.at[k], f, r, 1 - t)
    relay = n_r == 4
    near = [1, 2] if relay else js
    m2 = {}

    def pair(j):
        return lax.bitwise_xor(r, j) if relay else r_to(j)

    def spread_masters(k):
        m1[k].wait_recv()
        at = span(f_from(k) * rows + r * quarter, quarter, quarter)
        for j in near:
            m2[k, j] = send(masters_out.at[at], masters_out.at[at], m2s.at[k, j], m2r.at[k, j], f, pair(j), t)

    def relay_masters(k):
        for j in near:
            m2[k, j].wait_recv()
        if relay:
            part = quarter // 2
            for i, j in enumerate(near):
                start = f_from(k) * rows + pair(j) * quarter + i * part
                at = span(start, part, part)
                to = near[1 - i]
                slot = 0 if i == 0 else 3
                m2[k, slot] = send(masters_out.at[at], masters_out.at[at], m2s.at[k, slot], m2r.at[k, slot], f, pair(to), t)

    cut1 = (len(ks) + 2) // 3
    cut2 = (2 * len(ks) + 2) // 3
    for k in ks[:cut1]:
        spread_masters(k)
    for k in ks:
        f3[k].wait_recv()
        project(f_from(k), False)
    if not blocked:
        project(f, True)
    lfac = local(fac, factor_out, 12)

    for c in lc:
        c.wait()
    r1 = {}
    for g in range(2):
        turned = acc[:, g * rank:(g + 1) * rank].astype(BF).T
        part = jnp.dot(turned, cot_v[g], preferred_element_type=F32).astype(BF)
        for q in range(n_r):
            pbuf[q, g] = part[:, q * cw:(q + 1) * cw]
        for j in js:
            r1[j, g] = send(pbuf.at[r_to(j), g], r1buf.at[j, g], r1s.at[j, g], r1r.at[j, g], f, r_to(j), t)

    for k in ks[:cut1]:
        relay_masters(k)
    for k in ks[cut1:cut2]:
        spread_masters(k)

    for g in range(2):
        total = pbuf[r, g].astype(F32)
        for j in js:
            r1[j, g].wait_recv()
            total = total + r1buf[j, g].astype(F32)
        sumbuf[g] = total.astype(BF)
    r2 = {}
    for k in ks:
        r2[k] = send(
            sumbuf.at[:, span(f_to(k) * own, own, own), :], r2buf.at[k],
            r2s.at[k], r2r.at[k], f_to(k), r, t)
    low = sumbuf[:, span(f * own, own, own), :].astype(F32)
    for k in ks:
        r2[k].wait_recv()
        low = low + r2buf[k].astype(F32)
    for c in lo:
        c.wait()
    lall[r] = low.astype(BF)
    columns = span(r * cw, cw, cw)
    for g in range(2):
        first = 0.8 * old[2 * g, :, columns] + 0.2 * low[g]
        second = 0.95 * old[2 * g + 1, :, columns] + 0.05 * low[g] * low[g]
        nall[r, g, span(f * own, own, own), :] = (first / jnp.sqrt(second)).astype(BF)
    a1 = {}
    for k in ks:
        at = nall.at[r, :, span(f * own, own, own), :]
        a1[k] = send(at, at, a1s.at[k], a1r.at[k], f_to(k), r, t)
    al = {}
    for j in js:
        al[j] = send(lall.at[r], lall.at[r], als.at[j], alr.at[j], f, r_to(j), t)
    for k in ks[cut1:cut2]:
        relay_masters(k)
    for k in ks[cut2:]:
        spread_masters(k)
    for k in ks:
        a1[k].wait_recv()
    a2 = {}
    for j in js:
        a2[j] = send(nall.at[r], nall.at[r], a2s.at[j], a2r.at[j], f, r_to(j), t)
    for k in ks[cut2:]:
        relay_masters(k)
    for j in js:
        al[j].wait_recv()
    llow = local(lall, low_out, 13)
    for j in js:
        a2[j].wait_recv()
    lnorm = local(nall, normed_out, 14)

    for g in range(2):
        whole = jnp.concatenate([nall[q, g] for q in range(n_r)], axis=1)

        def square(i, total):
            at = span(i * 256, 256, 256)
            full = jnp.dot(fac[at, g * rank:(g + 1) * rank], whole, preferred_element_type=F32)
            return total + jnp.sum((full * full).reshape(32, 8, width), axis=0)

        total = lax.fori_loop(0, fac.shape[0] // 256, square, jnp.zeros((8, width), F32))
        part = total[:, :128]
        for q in range(1, width // 128):
            part = part + total[:, q * 128:(q + 1) * 128]
        sq[t, g] = part
    other = send(sq.at[t], sq.at[t], sqs, sqr, f, r, 1 - t)
    other.wait_recv()
    lsq = local(sq, square_out, 15)
    for c in (lown, lfac, llow, lnorm, lsq):
        c.wait()
    for k in ks:
        for j in ((0, 3) if relay else ()):
            m2[k, j].wait_recv()
    for c in sent:
        c.wait_send()


def finish_kernel(
    entries,
    fac, mas, nor, low, sqr, fi, fg, mi, mg, p0, s0, p1, s1,
    mi_new, mg_new, ui, ug, p0n, s0n, p1n, s1n, ci, cg,
):
    n_r = nor.shape[0]
    width = mi.shape[1]
    rank = fi.shape[1]
    new = ((p0, s0, p0n, s0n), (p1, s1, p1n, s1n))

    @pl.when(pl.program_id(0) == 0)
    def _():
        for g, (p, s, pn, sn) in enumerate(new):
            got = jnp.concatenate([low[q, g] for q in range(n_r)], axis=1).astype(F32)
            pn[...] = 0.8 * p[...] + 0.2 * got
            sn[...] = 0.95 * s[...] + 0.05 * got * got

    for g, (own_f, own_m, m_new, up, copy) in enumerate(((fi, mi, mi_new, ui, ci), (fg, mg, mg_new, ug, cg))):
        whole = jnp.concatenate([nor[q, g] for q in range(n_r)], axis=1)
        square = jnp.sum(sqr[0, g] + sqr[1, g], keepdims=True)
        scale = 1.0 / jnp.sqrt(square / entries + 0.1)
        full = jnp.dot(own_f[...], whole, preferred_element_type=F32)
        update = full * scale
        up[...] = update
        m_new[...] = own_m[...] - 0.05 * update
        rest = jnp.dot(fac[:, g * rank:(g + 1) * rank], whole, preferred_element_type=F32)
        base = mas[:, g * width:(g + 1) * width].astype(F32)
        copy[...] = (base - 0.05 * (rest * scale)).astype(BF)


def on_device(n_f, n_r, n_t, x, ci, cg, mi, mg, fi, fg, p0, s0, p1, s1):
    tokens, d = x.shape
    rows, width = mi.shape
    rank = fi.shape[1]
    own = p0.shape[0]
    cw = width // n_r
    any_ = pl.BlockSpec(memory_space=pl.ANY)
    dma = pltpu.SemaphoreType.DMA
    S = jax.ShapeDtypeStruct
    masters, factors, normed, low, squares = pl.pallas_call(
        functools.partial(exchange_kernel, n_f, n_r),
        out_shape=(
            S((d, 2 * width), BF),
            S((d, 2 * rank), BF),
            S((n_r, 2, rank, cw), BF),
            S((n_r, 2, own, cw), BF),
            S((2, 2, 8, 128), F32),
        ),
        in_specs=[any_] * 11,
        out_specs=(any_,) * 5,
        scratch_shapes=[
            pltpu.VMEM((tokens, d), BF),
            pltpu.VMEM((2, tokens, width), BF),
            pltpu.VMEM((d, 2 * rank), BF),
            pltpu.VMEM((2, rows, width), F32),
            pltpu.VMEM((rows, 2 * width), BF),
            pltpu.VMEM((4, own, width), F32),
            pltpu.VMEM((tokens, 2 * rank), F32),
            pltpu.VMEM((n_r, 2, rank, cw), BF),
            pltpu.VMEM((n_r, 2, rank, cw), BF),
            pltpu.VMEM((2, rank, cw), BF),
            pltpu.VMEM((n_f, 2, own, cw), BF),
            pltpu.VMEM((n_r, 2, rank, cw), BF),
            pltpu.VMEM((n_r, 2, own, cw), BF),
            pltpu.VMEM((2, 2, 8, 128), F32),
            dma((16,)),
            dma((n_f,)), dma((n_f,)),
            dma((n_f, n_r)), dma((n_f, n_r)),
            dma((n_f,)), dma((n_f,)),
            dma((n_f,)), dma((n_f,)),
            dma((n_f, n_r)), dma((n_f, n_r)),
            dma((n_r, 2)), dma((n_r, 2)),
            dma((n_f,)), dma((n_f,)),
            dma((n_f,)), dma((n_f,)),
            dma((n_r,)), dma((n_r,)),
            dma((n_r,)), dma((n_r,)),
            dma, dma,
        ],
        compiler_params=pltpu.CompilerParams(
            collective_id=0, has_side_effects=True, vmem_limit_bytes=LIMIT),
        name="exchange",
    )(x, ci, cg, mi, mg, fi, fg, p0, s0, p1, s1)

    steps = 8
    dt, rt = d // steps, rows // steps

    def tiled(a, b):
        return pl.BlockSpec((a, b), lambda i: (i, 0))

    def fixed(shape):
        return pl.BlockSpec(shape, lambda i: (0,) * len(shape))

    moment = fixed((own, width))
    return pl.pallas_call(
        functools.partial(finish_kernel, d * width * n_t),
        grid=(steps,),
        out_shape=(S((rows, width), F32),) * 4 + (S((own, width), F32),) * 4 + (S((d, width), BF),) * 2,
        in_specs=[
            tiled(dt, 2 * rank), tiled(dt, 2 * width),
            fixed(normed.shape), fixed(low.shape), fixed(squares.shape),
            tiled(rt, rank), tiled(rt, rank), tiled(rt, width), tiled(rt, width),
            moment, moment, moment, moment,
        ],
        out_specs=(tiled(rt, width),) * 4 + (moment,) * 4 + (tiled(dt, width),) * 2,
        compiler_params=pltpu.CompilerParams(
            dimension_semantics=("arbitrary",), vmem_limit_bytes=LIMIT),
        name="finish",
    )(factors, masters, normed, low, squares, fi, fg, mi, mg, p0, s0, p1, s1)


def solution(mesh):
    tokens = P(("fs", "rep"), None)
    cots = P(("fs", "rep"), "tp")
    both, tall, wide = P("fs", "tp"), P("fs", None), P(None, "tp")
    return jax.shard_map(
        functools.partial(on_device, mesh.shape["fs"], mesh.shape["rep"], mesh.shape["tp"]),
        mesh=mesh,
        in_specs=(tokens, cots, cots, both, both, tall, tall, both, both, both, both),
        out_specs=(both,) * 8 + (wide,) * 2,
        check_vma=False,
    )
```

```python
import functools

import jax
import jax.numpy as jnp
from jax import lax
from jax.experimental import pallas as pl
from jax.experimental.pallas import tpu as pltpu
from jax.sharding import PartitionSpec as P

MESH = pl.DeviceIdType.MESH
BF = jnp.bfloat16
F32 = jnp.float32
LIMIT = 60 * 1024 * 1024


def exchange_kernel(
    n_f, n_r,
    x_hbm, ci_hbm, cg_hbm, mi_hbm, mg_hbm, fi_hbm, fg_hbm, p0_hbm, s0_hbm, p1_hbm, s1_hbm,
    masters_out, factor_out, normed_out, low_out, square_out,
    x_v, cot_v, fac, mas32, mas16, old, acc, pbuf, r1buf, sumbuf, r2buf, nall, lall, sq,
    loc, f1s, f1r, f2s, f2r, f3s, f3r, m1s, m1r, m2s, m2r, r1s, r1r, r2s, r2r,
    a1s, a1r, als, alr, a2s, a2r, sqs, sqr,
):
    f, r, t = lax.axis_index("fs"), lax.axis_index("rep"), lax.axis_index("tp")
    tokens = x_v.shape[0]
    rows = mi_hbm.shape[0]
    width = mi_hbm.shape[1]
    rank = fi_hbm.shape[1]
    own = p0_hbm.shape[0]
    cw = width // n_r
    half = rows // 2
    piece = half // n_r
    quarter = rows // n_r
    ks = sorted(range(1, n_f), key=lambda k: min(k, n_f - k))
    js = list(range(1, n_r))

    def f_to(k):
        return lax.rem(f + k, n_f)

    def f_from(k):
        return lax.rem(f - k + n_f, n_f)

    def r_to(j):
        return lax.rem(r + j, n_r)

    def span(start, size, unit):
        return pl.ds(pl.multiple_of(start, unit), size)

    relay = n_r == 4
    near = [1, 2] if relay else js
    short = relay and piece % 16 == 0

    def pair(j):
        return lax.bitwise_xor(r, j) if relay else r_to(j)

    sent = []

    def send(src, dst, ss, rs, ff, rr, tt):
        c = pltpu.make_async_remote_copy(
            src_ref=src, dst_ref=dst, send_sem=ss, recv_sem=rs,
            device_id=(ff, rr, tt), device_id_type=MESH)
        c.start()
        sent.append(c)
        return c

    def local(src, dst, i):
        c = pltpu.make_async_copy(src, dst, loc.at[i])
        c.start()
        return c

    mine = span(f * rows, rows, rows)
    lf = [local(fi_hbm, fac.at[mine, pl.ds(0, rank)], 0), local(fg_hbm, fac.at[mine, pl.ds(rank, rank)], 1)]
    lm = [local(mi_hbm, mas32.at[0], 2), local(mg_hbm, mas32.at[1], 3)]
    lx = local(x_hbm, x_v, 4)
    lc = [local(ci_hbm, cot_v.at[0], 5), local(cg_hbm, cot_v.at[1], 6)]
    lo = [local(h, old.at[i], 7 + i) for i, h in enumerate((p0_hbm, s0_hbm, p1_hbm, s1_hbm))]

    barrier = pltpu.get_barrier_semaphore()
    for k in ks:
        pl.semaphore_signal(barrier, inc=1, device_id=(f_to(k), r, t), device_id_type=MESH)
    for j in js:
        for tt in (t, 1 - t):
            pl.semaphore_signal(barrier, inc=1, device_id=(f, r_to(j), tt), device_id_type=MESH)
    pl.semaphore_signal(barrier, inc=1, device_id=(f, r, 1 - t), device_id_type=MESH)
    pl.semaphore_wait(barrier, len(ks) + 2 * len(js) + 1)

    for c in lf:
        c.wait()
    f1 = {}
    for k in ks:
        at = span(f * rows + t * half + r * piece, piece, piece)
        f1[k] = send(fac.at[at], fac.at[at], f1s.at[k], f1r.at[k], f_to(k), r, t)
    for c in lm:
        c.wait()
    for g in range(2):
        mas16[:, g * width:(g + 1) * width] = mas32[g].astype(BF)
    m1 = {}
    for k in ks:
        m1[k] = send(
            mas16.at[span(r * quarter, quarter, quarter)],
            masters_out.at[span(f * rows + r * quarter, quarter, quarter)],
            m1s.at[k], m1r.at[k], f_to(k), r, t)
    lown = local(mas16, masters_out.at[mine], 11)
    lx.wait()

    tile = min(256, tokens)

    blocked = rows % 128 == 0

    def project(source, first):
        if not blocked and not first:
            return
        depth = span(source * rows, rows, rows) if blocked else slice(None)
        weights = fac[depth, :]

        def step(i, carry):
            at = span(i * tile, tile, tile)
            part = jnp.dot(x_v[at, depth], weights, preferred_element_type=F32)
            acc[at, :] = part if first else acc[at, :] + part
            return carry

        lax.fori_loop(0, tokens // tile, step, 0)

    f2 = {}

    def spread(k):
        f1[k].wait_recv()
        at = span(f_from(k) * rows + t * half + r * piece, piece, piece)
        for j in (near if short else js):
            to = pair(j) if short else r_to(j)
            f2[k, j] = send(fac.at[at], fac.at[at], f2s.at[k, j], f2r.at[k, j], f, to, t)

    if blocked:
        project(f, True)
    for k in ks:
        spread(k)
    f3 = {}
    if short:
        for k in ks:
            part = piece // 2
            for j in near:
                f2[k, j].wait_recv()
            for i, j in enumerate(near):
                at = span(f_from(k) * rows + t * half + pair(j) * piece + i * part, part, part)
                slot = 3 * i
                f2[k, slot] = send(fac.at[at], fac.at[at], f2s.at[k, slot], f2r.at[k, slot], f, pair(near[1 - i]), t)
    for k in ks:
        for j in ((0, 3) if short else js):
            f2[k, j].wait_recv()
        at = span(f_from(k) * rows + t * half, half, half)
        f3[k] = send(fac.at[at], fac.at[at], f3s.at[k], f3r.at[k], f, r, 1 - t)
    m2 = {}

    def spread_masters(k):
        m1[k].wait_recv()
        at = span(f_from(k) * rows + r * quarter, quarter, quarter)
        for j in near:
            m2[k, j] = send(masters_out.at[at], masters_out.at[at], m2s.at[k, j], m2r.at[k, j], f, pair(j), t)

    def relay_masters(k):
        for j in near:
            m2[k, j].wait_recv()
        if relay:
            part = quarter // 2
            for i, j in enumerate(near):
                start = f_from(k) * rows + pair(j) * quarter + i * part
                at = span(start, part, part)
                to = near[1 - i]
                slot = 0 if i == 0 else 3
                m2[k, slot] = send(masters_out.at[at], masters_out.at[at], m2s.at[k, slot], m2r.at[k, slot], f, pair(to), t)

    cut1 = (len(ks) + 2) // 3
    cut2 = (2 * len(ks) + 2) // 3
    for k in ks[:cut1]:
        spread_masters(k)
    for k in ks:
        f3[k].wait_recv()
        project(f_from(k), False)
    if not blocked:
        project(f, True)
    lfac = local(fac, factor_out, 12)

    for c in lc:
        c.wait()
    r1 = {}
    for g in range(2):
        turned = acc[:, g * rank:(g + 1) * rank].astype(BF).T
        part = jnp.dot(turned, cot_v[g], preferred_element_type=F32).astype(BF)
        for q in range(n_r):
            pbuf[q, g] = part[:, q * cw:(q + 1) * cw]
        for j in js:
            r1[j, g] = send(pbuf.at[r_to(j), g], r1buf.at[j, g], r1s.at[j, g], r1r.at[j, g], f, r_to(j), t)

    for k in ks[:cut1]:
        relay_masters(k)
    for k in ks[cut1:cut2]:
        spread_masters(k)

    for g in range(2):
        total = pbuf[r, g].astype(F32)
        for j in js:
            r1[j, g].wait_recv()
            total = total + r1buf[j, g].astype(F32)
        sumbuf[g] = total.astype(BF)
    r2 = {}
    for k in ks:
        r2[k] = send(
            sumbuf.at[:, span(f_to(k) * own, own, own), :], r2buf.at[k],
            r2s.at[k], r2r.at[k], f_to(k), r, t)
    low = sumbuf[:, span(f * own, own, own), :].astype(F32)
    for k in ks:
        r2[k].wait_recv()
        low = low + r2buf[k].astype(F32)
    for c in lo:
        c.wait()
    lall[r] = low.astype(BF)
    columns = span(r * cw, cw, cw)
    for g in range(2):
        first = 0.8 * old[2 * g, :, columns] + 0.2 * low[g]
        second = 0.95 * old[2 * g + 1, :, columns] + 0.05 * low[g] * low[g]
        nall[r, g, span(f * own, own, own), :] = (first / jnp.sqrt(second)).astype(BF)
    a1 = {}
    for k in ks:
        at = nall.at[r, :, span(f * own, own, own), :]
        a1[k] = send(at, at, a1s.at[k], a1r.at[k], f_to(k), r, t)
    al = {}
    for j in js:
        al[j] = send(lall.at[r], lall.at[r], als.at[j], alr.at[j], f, r_to(j), t)
    for k in ks[cut1:cut2]:
        relay_masters(k)
    for k in ks[cut2:]:
        spread_masters(k)
    for k in ks:
        a1[k].wait_recv()
    a2 = {}
    for j in near:
        a2[j] = send(nall.at[r], nall.at[r], a2s.at[j], a2r.at[j], f, pair(j), t)
    for g in range(2):
        quarter_g = nall[r, g]

        def square(i, total):
            at = span(i * 256, 256, 256)
            full = jnp.dot(fac[at, g * rank:(g + 1) * rank], quarter_g, preferred_element_type=F32)
            return total + jnp.sum((full * full).reshape(32, 8, cw), axis=0)

        sq[t, r, g] = lax.fori_loop(0, fac.shape[0] // 256, square, jnp.zeros((8, cw), F32))
    mysq = sq.at[t, r]
    qs = {}
    for j in range(n_r):
        for i, tt in enumerate((t, 1 - t)):
            if j or i:
                qs[j, i] = send(mysq, mysq, sqs.at[j, i], sqr.at[j, i], f, r_to(j), tt)
    if relay:
        for j in near:
            a2[j].wait_recv()
        for i, j in enumerate(near):
            at = nall.at[pair(j), i]
            slot = 3 * i
            a2[slot] = send(at, at, a2s.at[slot], a2r.at[slot], f, pair(near[1 - i]), t)
    for k in ks[cut2:]:
        relay_masters(k)
    for j in js:
        al[j].wait_recv()
    llow = local(lall, low_out, 13)
    for c in qs.values():
        c.wait_recv()
    lsq = local(sq, square_out, 15)
    for j in ((0, 3) if relay else js):
        a2[j].wait_recv()
    lnorm = local(nall, normed_out, 14)
    for c in (lown, lfac, llow, lnorm, lsq):
        c.wait()
    for k in ks:
        for j in ((0, 3) if relay else ()):
            m2[k, j].wait_recv()
    for c in sent:
        c.wait_send()


def finish_kernel(
    entries,
    fac, mas, nor, low, sqr, fi, fg, mi, mg, p0, s0, p1, s1,
    mi_new, mg_new, ui, ug, p0n, s0n, p1n, s1n, ci, cg,
):
    n_r = nor.shape[0]
    width = mi.shape[1]
    rank = fi.shape[1]
    new = ((p0, s0, p0n, s0n), (p1, s1, p1n, s1n))

    @pl.when(pl.program_id(0) == 0)
    def _():
        for g, (p, s, pn, sn) in enumerate(new):
            got = jnp.concatenate([low[q, g] for q in range(n_r)], axis=1).astype(F32)
            pn[...] = 0.8 * p[...] + 0.2 * got
            sn[...] = 0.95 * s[...] + 0.05 * got * got

    for g, (own_f, own_m, m_new, up, copy) in enumerate(((fi, mi, mi_new, ui, ci), (fg, mg, mg_new, ug, cg))):
        whole = jnp.concatenate([nor[q, g] for q in range(n_r)], axis=1)
        parts = sum(sqr[i, q, g] for i in range(2) for q in range(n_r))
        square = jnp.sum(parts, keepdims=True)
        scale = 1.0 / jnp.sqrt(square / entries + 0.1)
        full = jnp.dot(own_f[...], whole, preferred_element_type=F32)
        update = full * scale
        up[...] = update
        m_new[...] = own_m[...] - 0.05 * update
        rest = jnp.dot(fac[:, g * rank:(g + 1) * rank], whole, preferred_element_type=F32)
        base = mas[:, g * width:(g + 1) * width].astype(F32)
        copy[...] = (base - 0.05 * (rest * scale)).astype(BF)


def on_device(n_f, n_r, n_t, x, ci, cg, mi, mg, fi, fg, p0, s0, p1, s1):
    tokens, d = x.shape
    rows, width = mi.shape
    rank = fi.shape[1]
    own = p0.shape[0]
    cw = width // n_r
    any_ = pl.BlockSpec(memory_space=pl.ANY)
    dma = pltpu.SemaphoreType.DMA
    S = jax.ShapeDtypeStruct
    masters, factors, normed, low, squares = pl.pallas_call(
        functools.partial(exchange_kernel, n_f, n_r),
        out_shape=(
            S((d, 2 * width), BF),
            S((d, 2 * rank), BF),
            S((n_r, 2, rank, cw), BF),
            S((n_r, 2, own, cw), BF),
            S((2, n_r, 2, 8, cw), F32),
        ),
        in_specs=[any_] * 11,
        out_specs=(any_,) * 5,
        scratch_shapes=[
            pltpu.VMEM((tokens, d), BF),
            pltpu.VMEM((2, tokens, width), BF),
            pltpu.VMEM((d, 2 * rank), BF),
            pltpu.VMEM((2, rows, width), F32),
            pltpu.VMEM((rows, 2 * width), BF),
            pltpu.VMEM((4, own, width), F32),
            pltpu.VMEM((tokens, 2 * rank), F32),
            pltpu.VMEM((n_r, 2, rank, cw), BF),
            pltpu.VMEM((n_r, 2, rank, cw), BF),
            pltpu.VMEM((2, rank, cw), BF),
            pltpu.VMEM((n_f, 2, own, cw), BF),
            pltpu.VMEM((n_r, 2, rank, cw), BF),
            pltpu.VMEM((n_r, 2, own, cw), BF),
            pltpu.VMEM((2, n_r, 2, 8, cw), F32),
            dma((16,)),
            dma((n_f,)), dma((n_f,)),
            dma((n_f, n_r)), dma((n_f, n_r)),
            dma((n_f,)), dma((n_f,)),
            dma((n_f,)), dma((n_f,)),
            dma((n_f, n_r)), dma((n_f, n_r)),
            dma((n_r, 2)), dma((n_r, 2)),
            dma((n_f,)), dma((n_f,)),
            dma((n_f,)), dma((n_f,)),
            dma((n_r,)), dma((n_r,)),
            dma((n_r,)), dma((n_r,)),
            dma((n_r, 2)), dma((n_r, 2)),
        ],
        compiler_params=pltpu.CompilerParams(
            collective_id=0, has_side_effects=True, vmem_limit_bytes=LIMIT),
        name="exchange",
    )(x, ci, cg, mi, mg, fi, fg, p0, s0, p1, s1)

    steps = 8
    dt, rt = d // steps, rows // steps

    def tiled(a, b):
        return pl.BlockSpec((a, b), lambda i: (i, 0))

    def fixed(shape):
        return pl.BlockSpec(shape, lambda i: (0,) * len(shape))

    moment = fixed((own, width))
    return pl.pallas_call(
        functools.partial(finish_kernel, d * width * n_t),
        grid=(steps,),
        out_shape=(S((rows, width), F32),) * 4 + (S((own, width), F32),) * 4 + (S((d, width), BF),) * 2,
        in_specs=[
            tiled(dt, 2 * rank), tiled(dt, 2 * width),
            fixed(normed.shape), fixed(low.shape), fixed(squares.shape),
            tiled(rt, rank), tiled(rt, rank), tiled(rt, width), tiled(rt, width),
            moment, moment, moment, moment,
        ],
        out_specs=(tiled(rt, width),) * 4 + (moment,) * 4 + (tiled(dt, width),) * 2,
        compiler_params=pltpu.CompilerParams(
            dimension_semantics=("arbitrary",), vmem_limit_bytes=LIMIT),
        name="finish",
    )(factors, masters, normed, low, squares, fi, fg, mi, mg, p0, s0, p1, s1)


def solution(mesh):
    tokens = P(("fs", "rep"), None)
    cots = P(("fs", "rep"), "tp")
    both, tall, wide = P("fs", "tp"), P("fs", None), P(None, "tp")
    return jax.shard_map(
        functools.partial(on_device, mesh.shape["fs"], mesh.shape["rep"], mesh.shape["tp"]),
        mesh=mesh,
        in_specs=(tokens, cots, cots, both, both, tall, tall, both, both, both, both),
        out_specs=(both,) * 8 + (wide,) * 2,
        check_vma=False,
    )
```

```python
import functools

import jax
import jax.numpy as jnp
from jax import lax
from jax.experimental import pallas as pl
from jax.experimental.pallas import tpu as pltpu
from jax.sharding import PartitionSpec as P

MESH = pl.DeviceIdType.MESH
BF = jnp.bfloat16
F32 = jnp.float32
LIMIT = 60 * 1024 * 1024


def exchange_kernel(
    n_f, n_r,
    x_hbm, ci_hbm, cg_hbm, mi_hbm, mg_hbm, fi_hbm, fg_hbm, p0_hbm, s0_hbm, p1_hbm, s1_hbm,
    masters_out, factor_out, normed_out, low_out, square_out,
    x_v, cot_v, fac, mas32, mas16, old, acc, pbuf, r1buf, sumbuf, r2buf, nall, lall, sq,
    loc, f1s, f1r, f2s, f2r, f3s, f3r, m1s, m1r, m2s, m2r, r1s, r1r, r2s, r2r,
    a1s, a1r, als, alr, a2s, a2r, sqs, sqr,
):
    f, r, t = lax.axis_index("fs"), lax.axis_index("rep"), lax.axis_index("tp")
    tokens = x_v.shape[0]
    rows = mi_hbm.shape[0]
    width = mi_hbm.shape[1]
    rank = fi_hbm.shape[1]
    own = p0_hbm.shape[0]
    cw = width // n_r
    half = rows // 2
    piece = half // n_r
    quarter = rows // n_r
    ks = sorted(range(1, n_f), key=lambda k: min(k, n_f - k))
    js = list(range(1, n_r))

    def f_to(k):
        return lax.rem(f + k, n_f)

    def f_from(k):
        return lax.rem(f - k + n_f, n_f)

    def r_to(j):
        return lax.rem(r + j, n_r)

    def span(start, size, unit):
        return pl.ds(pl.multiple_of(start, unit), size)

    relay = n_r == 4
    near = [1, 2] if relay else js
    short = relay and piece % 16 == 0

    def pair(j):
        return lax.bitwise_xor(r, j) if relay else r_to(j)

    sent = []

    def send(src, dst, ss, rs, ff, rr, tt):
        c = pltpu.make_async_remote_copy(
            src_ref=src, dst_ref=dst, send_sem=ss, recv_sem=rs,
            device_id=(ff, rr, tt), device_id_type=MESH)
        c.start()
        sent.append(c)
        return c

    def local(src, dst, i):
        c = pltpu.make_async_copy(src, dst, loc.at[i])
        c.start()
        return c

    mine = span(f * rows, rows, rows)
    lf = [local(fi_hbm, fac.at[mine, pl.ds(0, rank)], 0), local(fg_hbm, fac.at[mine, pl.ds(rank, rank)], 1)]
    lm = [local(mi_hbm, mas32.at[0], 2), local(mg_hbm, mas32.at[1], 3)]
    lx = local(x_hbm, x_v, 4)
    lc = [local(ci_hbm, cot_v.at[0], 5), local(cg_hbm, cot_v.at[1], 6)]
    lo = [local(h, old.at[i], 7 + i) for i, h in enumerate((p0_hbm, s0_hbm, p1_hbm, s1_hbm))]

    barrier = pltpu.get_barrier_semaphore()
    for k in ks:
        pl.semaphore_signal(barrier, inc=1, device_id=(f_to(k), r, t), device_id_type=MESH)
    for j in js:
        for tt in (t, 1 - t):
            pl.semaphore_signal(barrier, inc=1, device_id=(f, r_to(j), tt), device_id_type=MESH)
    pl.semaphore_signal(barrier, inc=1, device_id=(f, r, 1 - t), device_id_type=MESH)
    pl.semaphore_wait(barrier, len(ks) + 2 * len(js) + 1)

    for c in lf:
        c.wait()
    f1 = {}
    for k in ks:
        at = span(f * rows + t * half + r * piece, piece, piece)
        f1[k] = send(fac.at[at], fac.at[at], f1s.at[k], f1r.at[k], f_to(k), r, t)
    for c in lm:
        c.wait()
    for g in range(2):
        mas16[:, g * width:(g + 1) * width] = mas32[g].astype(BF)
    m1 = {}
    for k in ks:
        m1[k] = send(
            mas16.at[span(r * quarter, quarter, quarter)],
            masters_out.at[span(f * rows + r * quarter, quarter, quarter)],
            m1s.at[k], m1r.at[k], f_to(k), r, t)
    lown = local(mas16, masters_out.at[mine], 11)
    lx.wait()

    tile = min(256, tokens)

    blocked = rows % 128 == 0

    def project(source, first):
        if not blocked and not first:
            return
        depth = span(source * rows, rows, rows) if blocked else slice(None)
        weights = fac[depth, :]

        def step(i, carry):
            at = span(i * tile, tile, tile)
            part = jnp.dot(x_v[at, depth], weights, preferred_element_type=F32)
            acc[at, :] = part if first else acc[at, :] + part
            return carry

        lax.fori_loop(0, tokens // tile, step, 0)

    f2 = {}

    def spread(k):
        f1[k].wait_recv()
        at = span(f_from(k) * rows + t * half + r * piece, piece, piece)
        for j in (near if short else js):
            to = pair(j) if short else r_to(j)
            f2[k, j] = send(fac.at[at], fac.at[at], f2s.at[k, j], f2r.at[k, j], f, to, t)

    if blocked:
        project(f, True)
    for k in ks:
        spread(k)
    f3 = {}
    if short:
        for k in ks:
            part = piece // 2
            for j in near:
                f2[k, j].wait_recv()
            for i, j in enumerate(near):
                at = span(f_from(k) * rows + t * half + pair(j) * piece + i * part, part, part)
                slot = 3 * i
                f2[k, slot] = send(fac.at[at], fac.at[at], f2s.at[k, slot], f2r.at[k, slot], f, pair(near[1 - i]), t)
    for k in ks:
        for j in ((0, 3) if short else js):
            f2[k, j].wait_recv()
        at = span(f_from(k) * rows + t * half, half, half)
        f3[k] = send(fac.at[at], fac.at[at], f3s.at[k], f3r.at[k], f, r, 1 - t)
    m2 = {}

    def spread_masters(k):
        m1[k].wait_recv()
        at = span(f_from(k) * rows + r * quarter, quarter, quarter)
        for j in near:
            m2[k, j] = send(masters_out.at[at], masters_out.at[at], m2s.at[k, j], m2r.at[k, j], f, pair(j), t)

    def relay_masters(k):
        for j in near:
            m2[k, j].wait_recv()
        if relay:
            part = quarter // 2
            for i, j in enumerate(near):
                start = f_from(k) * rows + pair(j) * quarter + i * part
                at = span(start, part, part)
                to = near[1 - i]
                slot = 0 if i == 0 else 3
                m2[k, slot] = send(masters_out.at[at], masters_out.at[at], m2s.at[k, slot], m2r.at[k, slot], f, pair(to), t)

    cut1 = (len(ks) + 2) // 3
    cut2 = (2 * len(ks) + 2) // 3
    for k in ks[:cut1]:
        spread_masters(k)
    for k in ks:
        f3[k].wait_recv()
        project(f_from(k), False)
    if not blocked:
        project(f, True)
    lfac = local(fac, factor_out, 12)

    for c in lc:
        c.wait()
    r1 = {}
    for g in range(2):
        turned = acc[:, g * rank:(g + 1) * rank].astype(BF).T
        part = jnp.dot(turned, cot_v[g], preferred_element_type=F32).astype(BF)
        for q in range(n_r):
            pbuf[q, g] = part[:, q * cw:(q + 1) * cw]
        for j in js:
            r1[j, g] = send(pbuf.at[r_to(j), g], r1buf.at[j, g], r1s.at[j, g], r1r.at[j, g], f, r_to(j), t)

    for k in ks[:cut1]:
        relay_masters(k)
    for k in ks[cut1:cut2]:
        spread_masters(k)

    for g in range(2):
        total = pbuf[r, g].astype(F32)
        for j in js:
            r1[j, g].wait_recv()
            total = total + r1buf[j, g].astype(F32)
        sumbuf[g] = total.astype(BF)
    r2 = {}
    for k in ks:
        r2[k] = send(
            sumbuf.at[:, span(f_to(k) * own, own, own), :], r2buf.at[k],
            r2s.at[k], r2r.at[k], f_to(k), r, t)
    low = sumbuf[:, span(f * own, own, own), :].astype(F32)
    for k in ks:
        r2[k].wait_recv()
        low = low + r2buf[k].astype(F32)
    for c in lo:
        c.wait()
    lall[r] = low.astype(BF)
    columns = span(r * cw, cw, cw)
    for g in range(2):
        first = 0.8 * old[2 * g, :, columns] + 0.2 * low[g]
        second = 0.95 * old[2 * g + 1, :, columns] + 0.05 * low[g] * low[g]
        nall[r, g, span(f * own, own, own), :] = (first / jnp.sqrt(second)).astype(BF)
    a1 = {}
    for k in ks:
        at = nall.at[r, :, span(f * own, own, own), :]
        a1[k] = send(at, at, a1s.at[k], a1r.at[k], f_to(k), r, t)
    al = {}
    for j in js:
        al[j] = send(lall.at[r], lall.at[r], als.at[j], alr.at[j], f, r_to(j), t)
    for k in ks[cut1:cut2]:
        relay_masters(k)
    for k in ks[cut2:]:
        spread_masters(k)
    for k in ks:
        a1[k].wait_recv()
    a2 = {}
    for j in near:
        a2[j] = send(nall.at[r], nall.at[r], a2s.at[j], a2r.at[j], f, pair(j), t)
    for g in range(2):
        quarter_g = nall[r, g]

        def square(i, total):
            at = span(i * 256, 256, 256)
            full = jnp.dot(fac[at, g * rank:(g + 1) * rank], quarter_g, preferred_element_type=F32)
            return total + jnp.sum((full * full).reshape(32, 8, cw), axis=0)

        sq[t, r, g] = lax.fori_loop(0, fac.shape[0] // 256, square, jnp.zeros((8, cw), F32))
    mysq = sq.at[t, r]
    qs = {}
    for j in range(n_r):
        for i, tt in enumerate((t, 1 - t)):
            if j or i:
                qs[j, i] = send(mysq, mysq, sqs.at[j, i], sqr.at[j, i], f, r_to(j), tt)
    if relay:
        for j in near:
            a2[j].wait_recv()
        for i, j in enumerate(near):
            at = nall.at[pair(j), i]
            slot = 3 * i
            a2[slot] = send(at, at, a2s.at[slot], a2r.at[slot], f, pair(near[1 - i]), t)
    for k in ks[cut2:]:
        relay_masters(k)
    for j in js:
        al[j].wait_recv()
    llow = local(lall, low_out, 13)
    for c in qs.values():
        c.wait_recv()
    lsq = local(sq, square_out, 15)
    for j in ((0, 3) if relay else js):
        a2[j].wait_recv()
    lnorm = local(nall, normed_out, 14)
    for c in (lown, lfac, llow, lnorm, lsq):
        c.wait()
    for k in ks:
        for j in ((0, 3) if relay else ()):
            m2[k, j].wait_recv()
    for c in sent:
        c.wait_send()


def finish_kernel(
    entries,
    fac, mas, nor, low, sqr, fi, fg, mi, mg, p0, s0, p1, s1,
    mi_new, mg_new, ui, ug, p0n, s0n, p1n, s1n, ci, cg,
):
    n_r = nor.shape[0]
    width = mi.shape[1]
    rank = fi.shape[1]
    new = ((p0, s0, p0n, s0n), (p1, s1, p1n, s1n))

    @pl.when(pl.program_id(0) == 0)
    def _():
        for g, (p, s, pn, sn) in enumerate(new):
            got = jnp.concatenate([low[q, g] for q in range(n_r)], axis=1).astype(F32)
            pn[...] = 0.8 * p[...] + 0.2 * got
            sn[...] = 0.95 * s[...] + 0.05 * got * got

    for g, (own_f, own_m, m_new, up, copy) in enumerate(((fi, mi, mi_new, ui, ci), (fg, mg, mg_new, ug, cg))):
        whole = jnp.concatenate([nor[q, g] for q in range(n_r)], axis=1)
        parts = sum(sqr[i, q, g] for i in range(2) for q in range(n_r))
        square = jnp.sum(parts, keepdims=True)
        scale = 1.0 / jnp.sqrt(square / entries + 0.1)
        full = jnp.dot(own_f[...], whole, preferred_element_type=F32)
        update = full * scale
        up[...] = update
        m_new[...] = own_m[...] - 0.05 * update
        rest = jnp.dot(fac[:, g * rank:(g + 1) * rank], whole, preferred_element_type=F32)
        base = mas[:, g * width:(g + 1) * width].astype(F32)
        copy[...] = (base - 0.05 * (rest * scale)).astype(BF)


def on_device(n_f, n_r, n_t, x, ci, cg, mi, mg, fi, fg, p0, s0, p1, s1):
    tokens, d = x.shape
    rows, width = mi.shape
    rank = fi.shape[1]
    own = p0.shape[0]
    cw = width // n_r
    any_ = pl.BlockSpec(memory_space=pl.ANY)
    dma = pltpu.SemaphoreType.DMA
    S = jax.ShapeDtypeStruct
    hx, hci, hcg, hmi, hmg, hfi, hfg, h0, h1, h2, h3 = (pltpu.with_memory_space_constraint(v, pltpu.HBM) for v in (x, ci, cg, mi, mg, fi, fg, p0, s0, p1, s1))
    masters, factors, normed, low, squares = pl.pallas_call(
        functools.partial(exchange_kernel, n_f, n_r),
        out_shape=(
            S((d, 2 * width), BF),
            S((d, 2 * rank), BF),
            S((n_r, 2, rank, cw), BF),
            S((n_r, 2, own, cw), BF),
            S((2, n_r, 2, 8, cw), F32),
        ),
        in_specs=[any_] * 11,
        out_specs=(any_,) * 5,
        scratch_shapes=[
            pltpu.VMEM((tokens, d), BF),
            pltpu.VMEM((2, tokens, width), BF),
            pltpu.VMEM((d, 2 * rank), BF),
            pltpu.VMEM((2, rows, width), F32),
            pltpu.VMEM((rows, 2 * width), BF),
            pltpu.VMEM((4, own, width), F32),
            pltpu.VMEM((tokens, 2 * rank), F32),
            pltpu.VMEM((n_r, 2, rank, cw), BF),
            pltpu.VMEM((n_r, 2, rank, cw), BF),
            pltpu.VMEM((2, rank, cw), BF),
            pltpu.VMEM((n_f, 2, own, cw), BF),
            pltpu.VMEM((n_r, 2, rank, cw), BF),
            pltpu.VMEM((n_r, 2, own, cw), BF),
            pltpu.VMEM((2, n_r, 2, 8, cw), F32),
            dma((16,)),
            dma((n_f,)), dma((n_f,)),
            dma((n_f, n_r)), dma((n_f, n_r)),
            dma((n_f,)), dma((n_f,)),
            dma((n_f,)), dma((n_f,)),
            dma((n_f, n_r)), dma((n_f, n_r)),
            dma((n_r, 2)), dma((n_r, 2)),
            dma((n_f,)), dma((n_f,)),
            dma((n_f,)), dma((n_f,)),
            dma((n_r,)), dma((n_r,)),
            dma((n_r,)), dma((n_r,)),
            dma((n_r, 2)), dma((n_r, 2)),
        ],
        compiler_params=pltpu.CompilerParams(
            collective_id=0, has_side_effects=True, vmem_limit_bytes=26*1024*1024),
        name="exchange",
    )(hx, hci, hcg, hmi, hmg, hfi, hfg, h0, h1, h2, h3)

    steps = 8
    dt, rt = d // steps, rows // steps

    def tiled(a, b):
        return pl.BlockSpec((a, b), lambda i: (i, 0))

    def fixed(shape):
        return pl.BlockSpec(shape, lambda i: (0,) * len(shape))

    moment = fixed((own, width))
    return pl.pallas_call(
        functools.partial(finish_kernel, d * width * n_t),
        grid=(steps,),
        out_shape=(S((rows, width), F32),) * 4 + (S((own, width), F32),) * 4 + (S((d, width), BF),) * 2,
        in_specs=[
            tiled(dt, 2 * rank), tiled(dt, 2 * width),
            fixed(normed.shape), fixed(low.shape), fixed(squares.shape),
            tiled(rt, rank), tiled(rt, rank), tiled(rt, width), tiled(rt, width),
            moment, moment, moment, moment,
        ],
        out_specs=(tiled(rt, width),) * 4 + (moment,) * 4 + (tiled(dt, width),) * 2,
        compiler_params=pltpu.CompilerParams(
            dimension_semantics=("arbitrary",), vmem_limit_bytes=26*1024*1024),
        name="finish",
    )(factors, masters, normed, low, squares, fi, fg, mi, mg, p0, s0, p1, s1)


def solution(mesh):
    tokens = P(("fs", "rep"), None)
    cots = P(("fs", "rep"), "tp")
    both, tall, wide = P("fs", "tp"), P("fs", None), P(None, "tp")
    return jax.shard_map(
        functools.partial(on_device, mesh.shape["fs"], mesh.shape["rep"], mesh.shape["tp"]),
        mesh=mesh,
        in_specs=(tokens, cots, cots, both, both, tall, tall, both, both, both, both),
        out_specs=(both,) * 8 + (wide,) * 2,
        check_vma=False,
    )
```
